32 devices in a mesh: sp: 16 (over z, y, x), tp: 2 (over core).
Axes of the slice: x: 2, y: 2, z: 4, core: 2. Of those that a mesh axis runs over, the one named last changes fastest.
Arguments:
- tokens: bfloat16 [4096, 2048], P(('sp', 'tp')), may hold values from -6 to 6
- documents: int32 [4096], P('sp'), may hold values from 0 to 3, never falling along the last dimension, each value on 1 to 2048 neighbouring positions
- w_query: bfloat16 [2, 2048, 512], P(None, None, 'tp'), may hold values from -0.125 to 0.125
- w_key: bfloat16 [2, 2048, 256], P(None, None, 'tp'), may hold values from -0.125 to 0.125
- w_value: bfloat16 [2, 2048, 256], P(None, None, 'tp'), may hold values from -0.125 to 0.125
- w_out: bfloat16 [2, 512, 2048], P(None, 'tp'), may hold values from -0.25 to 0.25
- rel_table: float32 [2, 8, 257], P(None, 'tp'), may hold values from -250 to 250
- norm_gain: float32 [2, 2048], replicated, may hold values from 0.1 to 1.9
- norm_shift: float32 [2, 2048], replicated, may hold values from -3 to 3
Outputs:
- encoded: bfloat16 [4096, 2048], P(('sp', 'tp'))
The draws below stay inside these ranges and needn't reach their ends.
Inputs may be any that keep to these rules, and one draw needn't show every extreme that they name: `documents`: document numbers never fall along the sequence; a document spans at most 2048 positions.
All inputs are finite; a program needn't handle non-finite values.
Results may differ from the reference program's by a relative error of at most 0.0075.
Values may be sent and summed in bfloat16 or wider, within the bound.
A program may use at most 64 MiB of HBM per device.

```python
import math
import jax
import jax.numpy as jnp
import numpy as np
from jax import lax

D = 2048
HEADS = 8
KV_HEADS = 4
HD = 64
SEG = 64
LEFT = 4
CLIP = 128
LAYERS = 2
TOK_DEV = 256
TOKENS = 4096
ATTN = 512
KV_WIDTH = 256
DOCS = 4
N_TP = 2


def draw_rel_table(key, part):
    shape = (LAYERS, HEADS, 2 * CLIP + 1)
    table = jax.random.normal(key, shape, jnp.float32)
    return table


def levels(key, extent, cuts, least, high):
    def one(dim, blocks):
        heights = jax.random.uniform(jax.random.fold_in(jax.random.fold_in(key, 6), dim), (blocks,), jnp.float32, least / len(cuts), high / len(cuts))
        return jnp.repeat(jnp.exp(heights), extent[dim] // blocks).reshape((-1,) + (1,) * (len(extent) - dim - 1))

    factor_of = one(*cuts[0])
    for cut in cuts[1:]:
        factor_of = factor_of * one(*cut)
    return factor_of


def length_profile(count, total, limit, lean):
    loads = [(1 << 20) // math.isqrt(rank ** lean) + 1 for rank in range(2, count + 1)]
    spare, given = total - limit - (count - 1), [1] * (count - 1)
    while spare > 0:
        free = [i for i in range(count - 1) if given[i] < limit]
        whole, left = sum([loads[i] for i in free]), spare
        for i in free:
            extra = min(limit - given[i], max(1, left * loads[i] // whole), spare)
            given[i] = given[i] + extra
            spare = spare - extra
    return np.array([limit] + given)


def uneven(stream_key, count, total, most, skew):
    if count == 2:
        one = jax.random.randint(stream_key, (), max(1, total - most), min(most, total - 1) + 1)
        return jnp.stack([one, total - one])
    tallies = jnp.asarray(length_profile(count, total, most, skew), jnp.int32)
    twos = (count - 1) // 2
    source_of, sink = tallies[1:1 + 2 * twos:2], tallies[2:2 + 2 * twos:2]
    slack = jnp.minimum(source_of - 1, most - sink)
    shifted = jax.random.randint(jax.random.fold_in(stream_key, 1), (twos,), 0, 1 << 20) % (slack + 1)
    tallies = tallies.at[1:1 + 2 * twos:2].set(source_of - shifted).at[2:2 + 2 * twos:2].set(sink + shifted)
    return tallies[jax.random.permutation(jax.random.fold_in(stream_key, 2), count)]


def noise(rng, dims, deviation, bound, cuts=(), kind=jnp.bfloat16):
    gain = levels(rng, dims, cuts, -0.22, 0.18) if cuts else 1.0
    entries = jax.random.normal(rng, dims, jnp.float32) * deviation * gain
    return jnp.minimum(jnp.maximum(entries, -bound), bound).astype(kind)


def setup_inputs(seed: int = 0) -> dict:
    keys = jax.random.split(jax.random.key(seed), 10)
    return {
        "tokens": noise(keys[0], (TOKENS, D), 1.0, 6.0, ((0, 32),)),
        "documents": jnp.searchsorted(jnp.cumsum(uneven(keys[1], DOCS, TOKENS, 8 * TOK_DEV, 1)), jnp.arange(TOKENS), side="right").astype(jnp.int32),
        "w_query": noise(keys[2], (LAYERS, D, ATTN), D ** -0.5, 0.125, ((2, 2),)),
        "w_key": noise(keys[3], (LAYERS, D, KV_WIDTH), D ** -0.5, 0.125, ((2, 2),)),
        "w_value": noise(keys[4], (LAYERS, D, KV_WIDTH), D ** -0.5, 0.125, ((2, 2),)),
        "w_out": noise(keys[5], (LAYERS, ATTN, D), ATTN ** -0.5, 0.25, ((1, 2),)),
        "rel_table": draw_rel_table(jax.random.fold_in(keys[9], 71), 0),
        "norm_gain": jnp.clip(1.0 + 0.18 * jax.random.normal(keys[7], (LAYERS, D), jnp.float32), 0.1, 1.9),
        "norm_shift": noise(keys[8], (LAYERS, D), 0.5, 3.0, (), jnp.float32),
    }


def banded(values, seg_count):
    pieces = values.reshape((seg_count + LEFT, SEG) + values.shape[1:])
    return jnp.concatenate([pieces[offset:offset + seg_count] for offset in range(LEFT + 1)], axis=1)

def attend(queries, key_rows, value_rows, documents, table):
    reach_len = LEFT * SEG
    band_len = reach_len + SEG
    group_size = HEADS // KV_HEADS
    seg_total = TOKENS // SEG
    per_step = math.gcd(seg_total, 16)
    key_pad = jnp.pad(key_rows, ((reach_len, 0), (0, 0)))
    value_pad = jnp.pad(value_rows, ((reach_len, 0), (0, 0)))
    doc_pad = jnp.pad(documents, (reach_len, 0), constant_values=-1)
    offsets = jnp.clip(jnp.arange(SEG)[:, None] + reach_len - jnp.arange(band_len)[None, :], -CLIP, CLIP) + CLIP
    bias = table.astype(jnp.float32)[:, offsets].reshape(KV_HEADS, group_size, SEG, band_len)

    def one_block(index):
        first = (index * per_step * SEG).astype(jnp.int32)
        span_len = per_step * SEG + reach_len
        q_blocks = lax.dynamic_slice_in_dim(queries, first, per_step * SEG, 0).astype(jnp.float32)
        q_blocks = q_blocks.reshape(per_step, SEG, KV_HEADS, group_size, HD)
        key_span = lax.dynamic_slice_in_dim(key_pad, first, span_len, 0).reshape(span_len, KV_HEADS, HD)
        value_span = lax.dynamic_slice_in_dim(value_pad, first, span_len, 0).reshape(span_len, KV_HEADS, HD)
        doc_span = lax.dynamic_slice_in_dim(doc_pad, first, span_len, 0)
        key_band = banded(key_span, per_step).astype(jnp.float32)
        value_band = banded(value_span, per_step).astype(jnp.float32)
        doc_band = banded(doc_span, per_step)
        doc_query = lax.dynamic_slice_in_dim(documents, first, per_step * SEG, 0).reshape(per_step, SEG)
        scores = jnp.einsum('nqkgd,nbkd->nkgqb', q_blocks, key_band) * HD ** (-0.5) + bias
        valid = doc_query[:, :, None] == doc_band[:, None, :]
        scores = jnp.where(valid[:, None, None], scores, -1e+30)
        peak = lax.optimization_barrier(jnp.max(scores, axis=-1, keepdims=True))
        expo = jnp.exp(scores - peak)
        weights = (expo / lax.optimization_barrier(jnp.sum(expo, axis=-1, keepdims=True))).astype(jnp.bfloat16)
        result = jnp.einsum('nkgqb,nbkd->nqkgd', weights.astype(jnp.float32), value_band)
        return result.astype(jnp.bfloat16).reshape(per_step * SEG, HEADS * HD)
    blocks = lax.map(one_block, jnp.arange(seg_total // per_step, dtype=jnp.int32))
    return blocks.reshape(TOKENS, HEADS * HD)

def reference(tokens, documents, w_query, w_key, w_value, w_out, rel_table, norm_gain, norm_shift):
    stream = tokens
    scale_res = (2.0 * LAYERS) ** 0.25
    part_cols = HEADS * HD // N_TP
    for depth in range(LAYERS):
        queries = jnp.dot(stream, w_query[depth], preferred_element_type=jnp.float32).astype(jnp.bfloat16)
        key_rows = jnp.dot(stream, w_key[depth], preferred_element_type=jnp.float32).astype(jnp.bfloat16)
        value_rows = jnp.dot(stream, w_value[depth], preferred_element_type=jnp.float32).astype(jnp.bfloat16)
        attended = attend(queries, key_rows, value_rows, documents, rel_table[depth])
        mixture = jnp.zeros((TOKENS, D), jnp.float32)
        for head_group in range(N_TP):
            partial_value = jnp.dot(attended[:, head_group * part_cols:(head_group + 1) * part_cols], w_out[depth][head_group * part_cols:(head_group + 1) * part_cols], preferred_element_type=jnp.float32).astype(jnp.bfloat16)
            partial_value = lax.optimization_barrier(partial_value)
            mixture = mixture + partial_value.astype(jnp.float32)
        residual = scale_res * stream.astype(jnp.float32) + mixture
        average = lax.optimization_barrier(jnp.mean(residual, axis=-1, keepdims=True))
        centred = residual - average
        spread = lax.optimization_barrier(jnp.mean(centred * centred, axis=-1, keepdims=True))
        normed = centred * lax.rsqrt(spread + 1e-05) * norm_gain[depth] + norm_shift[depth]
        stream = normed.astype(jnp.bfloat16)
    return stream
```

```python
import functools

import jax
import jax.numpy as jnp
from jax import lax
from jax.experimental import pallas as pl
from jax.experimental.pallas import tpu as pltpu
from jax.sharding import PartitionSpec as P

HD = 64
SEG = 64
LEFT = 4
CLIP = 128
MESH = pl.DeviceIdType.MESH
F32 = jnp.float32
BF16 = jnp.bfloat16


def kernel(n_sp, tok_h, doc_h, wq_h, wk_h, wv_h, wo_h, tbl_h, gain_h, shift_h, out,
           x, res, wq, wkv, wo, tbl, gain, shift, doc_own, doc_prev, kv, qst, bias, att, stat, begun,
           loc_sem, w_send, w_recv, s_send, s_recv, kv_send, kv_recv):
    sp = lax.axis_index("sp")
    tp = lax.axis_index("tp")
    other = 1 - tp
    layers = wq.shape[0]
    rows = x.shape[0]
    has_next = sp < n_sp - 1
    has_prev = sp > 0
    scale_res = (2.0 * layers) ** 0.25

    def local(src, dst, i):
        copy = pltpu.make_async_copy(src, dst, loc_sem.at[i])
        copy.start()
        return copy

    c_wkv, c_wq, c_wo = [], [], []
    for l in range(layers):
        base = 6 + 4 * l
        if l == 0:
            c_x = local(tok_h, x, 0)
        c_wkv.append((local(wk_h.at[l], wkv.at[l, tp, :, 0:2 * HD], base),
                      local(wv_h.at[l], wkv.at[l, tp, :, 2 * HD:4 * HD], base + 1)))
        if l == 0:
            c_doc = local(doc_h, doc_own, 1)
            c_tbl = local(tbl_h, tbl.at[tp], 2)
        c_wq.append(local(wq_h.at[l], wq.at[l, tp], base + 2))
        c_wo.append(local(wo_h.at[l], wo.at[l, tp], base + 3))
        if l == 0:
            c_gain = local(gain_h, gain, 3)
            c_shift = local(shift_h, shift, 4)

    barrier = pltpu.get_barrier_semaphore()

    def greet(dev_sp, dev_tp):
        pl.semaphore_signal(barrier, inc=1, device_id=(dev_sp, dev_tp), device_id_type=MESH)

    greet(sp, other)

    @pl.when(has_prev)
    def _():
        greet(sp - 1, tp)

    @pl.when(jnp.logical_not(has_prev))
    def _():
        doc_prev[...] = jnp.full_like(doc_prev, -1)
        for l in range(layers):
            for h in range(2):
                kv[l, h, 0:rows, :] = jnp.zeros((rows, 4 * HD), BF16)

        @pl.when(tp == 0)
        def _():
            for l in range(layers):
                for h in range(2):
                    kv[l, h, rows:2 * rows, :] = jnp.zeros((rows, 4 * HD), BF16)

    pl.semaphore_wait(barrier, jnp.where(has_next, 2, 1))

    def wcopy(ref, l, kind, half):
        return pltpu.make_async_remote_copy(
            src_ref=ref.at[l, half], dst_ref=ref.at[l, half],
            send_sem=w_send.at[l, kind], recv_sem=w_recv.at[l, kind],
            device_id=(sp, other), device_id_type=MESH)

    def send_w(ref, l, kind):
        wcopy(ref, l, kind, tp).start()

    def await_w(ref, l, kind):
        wcopy(ref, l, kind, other).wait_recv()

    def tbl_copy(half):
        return pltpu.make_async_remote_copy(
            src_ref=tbl.at[half], dst_ref=tbl.at[half], send_sem=s_send.at[0], recv_sem=s_recv.at[0],
            device_id=(sp, other), device_id_type=MESH)

    def doc_copy():
        return pltpu.make_async_remote_copy(
            src_ref=doc_own, dst_ref=doc_prev, send_sem=s_send.at[1], recv_sem=s_recv.at[1],
            device_id=(sp + 1, tp), device_id_type=MESH)

    def block(l, half, slot):
        return kv.at[l, half, pl.ds(slot * rows, rows), :]

    def kv_copy(l, half, src, slot, dev_sp, dev_tp):
        return pltpu.make_async_remote_copy(
            src_ref=block(l, half, src), dst_ref=block(l, half, slot),
            send_sem=kv_send.at[l, half, slot], recv_sem=kv_recv.at[l, half, slot],
            device_id=(dev_sp, dev_tp), device_id_type=MESH)

    def send_kv(l, half):
        @pl.when(has_next)
        def _():
            kv_copy(l, half, 2, 0, sp + 1, tp).start()

        @pl.when(tp == 0)
        def _():
            kv_copy(l, half, 2, 1, sp, 1).start()

    def await_kv(l, half):
        @pl.when(has_prev)
        def _():
            kv_copy(l, half, 2, 0, sp, other).wait_recv()

            @pl.when(tp == 1)
            def _():
                kv_copy(l, half, 0, 1, sp, 0).start()

        @pl.when((tp == 1) | has_prev)
        def _():
            kv_copy(l, half, 2, 1, sp, other).wait_recv()

    def await_sent_kv(l, half):
        @pl.when(has_next)
        def _():
            kv_copy(l, half, 2, 0, sp, other).wait_send()

        @pl.when((tp == 0) | has_prev)
        def _():
            kv_copy(l, half, 2, 1, sp, other).wait_send()

    def make_kv(l, half):
        y = jnp.dot(x[...], wkv[l, half], preferred_element_type=F32)
        kv[l, half, 2 * rows:3 * rows, :] = y.astype(BF16)

    lane = lax.broadcasted_iota(jnp.int32, (rows, 2 * HD), 1)
    low = lane < HD

    def make_q(l, half):
        y = jnp.dot(x[...], wq[l, half], preferred_element_type=F32)
        y = y.astype(BF16).astype(F32) * (HD ** -0.5)
        for j in range(2):
            pair = y[:, 2 * HD * j:2 * HD * (j + 1)]
            turned = pltpu.roll(pair, HD, 1)
            if j == 0:
                first, second = jnp.where(low, pair, 0.0), jnp.where(low, turned, 0.0)
            else:
                first, second = jnp.where(low, 0.0, turned), jnp.where(low, 0.0, pair)
            qst[2 * half + j, 0:rows, :] = first.astype(BF16)
            qst[2 * half + j, rows:2 * rows, :] = second.astype(BF16)

    def make_bias():
        first = tp == 0
        dp = doc_prev[...].astype(F32)
        do = doc_own[...].astype(F32)
        k0 = jnp.where(first, dp[0:1], dp[1:2])
        k1 = jnp.where(first, dp[1:2], do[0:1])
        k2 = jnp.where(first, do[0:1], do[1:2])
        e = lax.broadcasted_iota(jnp.int32, (rows, rows), 0)
        r = lax.broadcasted_iota(jnp.int32, (rows, rows), 1)
        shape = (rows, rows)
        queries = jnp.broadcast_to(k2, shape)
        same = [jnp.broadcast_to(k, shape).T == queries for k in (k0, k1, k2)]
        valid = [same[0] & ((e >= SEG) | (r < SEG)), same[1], same[2] & ((e < SEG) | (r >= SEG))]
        for l in range(layers):
            for head in range(8):
                half, i = head // 4, head % 4
                t0 = jnp.broadcast_to(tbl[half, l, i:i + 1, 0:CLIP], shape)
                t1 = jnp.broadcast_to(tbl[half, l, i:i + 1, CLIP:2 * CLIP], shape)
                c = jnp.broadcast_to(tbl[half, l, i:i + 1, 2 * CLIP:2 * CLIP + 1], shape)
                b1 = pltpu.roll(jnp.concatenate([c, t1], axis=1), 0, 1, stride=1, stride_axis=0)[:, :rows]
                b2 = pltpu.roll(jnp.concatenate([t1, t0], axis=1), 0, 1, stride=1, stride_axis=0)[:, :rows]
                cols = slice((head % 2) * rows, (head % 2 + 1) * rows)
                for k, b in enumerate((c, b1, b2)):
                    bias[l, head // 2, k * rows:(k + 1) * rows, cols] = jnp.where(valid[k], b, -1e30)

    def part(l, half, j, keys):
        s = lax.dot_general(kv[l, half, keys, 0:2 * HD], qst[2 * half + j], (((1,), (1,)), ((), ())),
                            preferred_element_type=F32)
        return s + bias[l, 2 * half + j, keys, :]

    def weigh(l, half, j, keys, p):
        o = lax.dot_general(kv[l, half, keys, 2 * HD:4 * HD], p.astype(BF16), (((0,), (0,)), ((), ())),
                            preferred_element_type=F32)
        return o[HD * j:HD * (j + 1), :]

    near, far = slice(2 * rows, 3 * rows), slice(0, 2 * rows)

    def attend_own(l, half):
        for j in range(2):
            g = 2 * half + j
            s = part(l, half, j, near)
            peak = jnp.max(s, axis=0, keepdims=True)
            p = jnp.exp(s - peak)
            stat[g, 0:1, :] = peak
            stat[g, 1:2, :] = jnp.sum(p, axis=0, keepdims=True)
            begun[g] = weigh(l, half, j, near, p)

    def attend(l, half):
        for j in range(2):
            g = 2 * half + j
            s = part(l, half, j, far)
            before = stat[g, 0:1, :]
            peak = jnp.maximum(jnp.max(s, axis=0, keepdims=True), before)
            fade = jnp.exp(before - peak)
            p = jnp.exp(s - peak)
            total = jnp.sum(p, axis=0, keepdims=True) + fade * stat[g, 1:2, :]
            o = (weigh(l, half, j, far, p) + fade * begun[g]) / total
            both = jnp.concatenate([o[:, 0:rows], o[:, rows:2 * rows]], axis=0)
            att[:, 2 * HD * g:2 * HD * (g + 1)] = both.T.astype(BF16)

    width = x.shape[1]
    step = 256

    def project(l):
        a = att[...]
        kd = wo.shape[2]

        def body(i, _):
            cols = pl.ds(pl.multiple_of(i * step, step), step)
            y = jnp.dot(a[:, 0:kd], wo[l, 0, :, cols], preferred_element_type=F32)
            y = y + jnp.dot(a[:, kd:2 * kd], wo[l, 1, :, cols], preferred_element_type=F32)
            res[:, cols] = scale_res * x[:, cols].astype(F32) + y
            return 0

        lax.fori_loop(0, width // step, body, 0, unroll=True)

    def normalise(l, dst):
        def body(i, _):
            rr = pl.ds(pl.multiple_of(i * 16, 16), 16)
            y = res[rr, :]
            mean = jnp.mean(y, axis=-1, keepdims=True)
            y = y - mean
            var = jnp.mean(y * y, axis=-1, keepdims=True)
            y = y * lax.rsqrt(var + 1e-5) * gain[l:l + 1, :] + shift[l:l + 1, :]
            dst[rr, :] = y.astype(BF16)
            return 0

        lax.fori_loop(0, rows // 16, body, 0, unroll=2)

    c_wkv[0][0].wait()
    c_wkv[0][1].wait()
    send_w(wkv, 0, 0)
    c_doc.wait()

    @pl.when(has_next)
    def _():
        doc_copy().start()

    c_tbl.wait()
    tbl_copy(tp).start()
    c_x.wait()
    make_kv(0, tp)
    c_wq[0].wait()
    send_w(wq, 0, 1)
    send_kv(0, tp)
    make_q(0, tp)
    await_w(wkv, 0, 0)
    make_kv(0, other)
    c_wo[0].wait()
    send_w(wo, 0, 2)
    send_kv(0, other)
    for l in range(1, layers):
        c_wkv[l][0].wait()
        c_wkv[l][1].wait()
        send_w(wkv, l, 0)
        c_wq[l].wait()
        send_w(wq, l, 1)
        c_wo[l].wait()
        send_w(wo, l, 2)
    tbl_copy(other).wait_recv()

    @pl.when(has_prev)
    def _():
        doc_copy().wait_recv()

    make_bias()
    await_w(wq, 0, 1)
    make_q(0, other)
    c_gain.wait()
    c_shift.wait()
    for l in range(layers):
        if l > 0:
            await_w(wkv, l, 0)
            await_w(wq, l, 1)

            @pl.when(tp == 0)
            def _():
                make_q(l, 0)

            make_kv(l, 0)
            send_kv(l, 0)
            make_kv(l, 1)
            send_kv(l, 1)
            make_q(l, 1)

            @pl.when(tp == 1)
            def _():
                make_q(l, 0)

        attend_own(l, 0)
        attend_own(l, 1)
        for h in ((1, 0) if l == 0 else (0, 1)):
            await_kv(l, h)
            attend(l, h)
        await_w(wo, l, 2)
        project(l)
        normalise(l, x if l < layers - 1 else out)

    for l in range(layers):
        for kind, ref in enumerate((wkv, wq, wo)):
            wcopy(ref, l, kind, tp).wait_send()
        for h in range(2):
            await_sent_kv(l, h)
    tbl_copy(tp).wait_send()

    @pl.when(has_next)
    def _():
        doc_copy().wait_send()


def solution(mesh):
    n_sp = mesh.shape["sp"]

    def shards(tokens, documents, w_query, w_key, w_value, w_out, rel_table, norm_gain, norm_shift):
        rows, width = tokens.shape
        layers = w_query.shape[0]
        docs = documents.reshape(2, rows)
        anywhere = pl.BlockSpec(memory_space=pl.ANY)
        return pl.pallas_call(
            functools.partial(kernel, n_sp),
            out_shape=pltpu.VMEM((rows, width), BF16),
            in_specs=[anywhere] * 9,
            out_specs=pl.BlockSpec(memory_space=pltpu.VMEM),
            scratch_shapes=[
                pltpu.VMEM((rows, width), BF16),
                pltpu.VMEM((rows, width), F32),
                pltpu.VMEM((layers, 2, width, w_query.shape[2]), BF16),
                pltpu.VMEM((layers, 2, width, 2 * w_key.shape[2]), BF16),
                pltpu.VMEM((layers, 2, w_out.shape[1], width), BF16),
                pltpu.VMEM((2,) + rel_table.shape, F32),
                pltpu.VMEM((layers, width), F32),
                pltpu.VMEM((layers, width), F32),
                pltpu.VMEM((2, rows), jnp.int32),
                pltpu.VMEM((2, rows), jnp.int32),
                pltpu.VMEM((layers, 2, 3 * rows, 4 * HD), BF16),
                pltpu.VMEM((4, 2 * rows, 2 * HD), BF16),
                pltpu.VMEM((layers, 4, 3 * rows, 2 * rows), F32),
                pltpu.VMEM((rows, 2 * w_out.shape[1]), BF16),
                pltpu.VMEM((4, 8, 2 * rows), F32),
                pltpu.VMEM((4, HD, 2 * rows), F32),
                pltpu.SemaphoreType.DMA((6 + 4 * layers,)),
                pltpu.SemaphoreType.DMA((layers, 3)),
                pltpu.SemaphoreType.DMA((layers, 3)),
                pltpu.SemaphoreType.DMA((2,)),
                pltpu.SemaphoreType.DMA((2,)),
                pltpu.SemaphoreType.DMA((layers, 2, 2)),
                pltpu.SemaphoreType.DMA((layers, 2, 2)),
            ],
            compiler_params=pltpu.CompilerParams(
                collective_id=0, has_side_effects=True, vmem_limit_bytes=60 * 1024 * 1024
            ),
        )(tokens, docs, w_query, w_key, w_value, w_out, rel_table, norm_gain, norm_shift)

    in_specs = (
        P(("sp", "tp"), None),
        P("sp"),
        P(None, None, "tp"),
        P(None, None, "tp"),
        P(None, None, "tp"),
        P(None, "tp", None),
        P(None, "tp", None),
        P(),
        P(),
    )
    return jax.shard_map(shards, mesh=mesh, in_specs=in_specs, out_specs=P(("sp", "tp"), None), check_vma=False)
```
